32 devices in a mesh: ep: 16 (over z, y, x), tp: 2 (over core).
Axes of the slice: x: 2, y: 2, z: 4, core: 2. Of those that a mesh axis runs over, the one named last changes fastest.
Arguments:
- tokens: bfloat16 [512, 2048], P('ep'), may hold values from -6 to 6
- mix_gain: float32 [2048], replicated, may hold values from 0.1 to 1.9
- w_query: bfloat16 [2048, 512], P('ep', 'tp'), may hold values from -0.125 to 0.125
- w_key: bfloat16 [2048, 512], P('ep', 'tp'), may hold values from -0.125 to 0.125
- w_value: bfloat16 [2048, 512], P('ep', 'tp'), may hold values from -0.125 to 0.125
- w_outgate: bfloat16 [2048, 512], P('ep', 'tp'), may hold values from -0.125 to 0.125
- w_igate: bfloat16 [2048, 8], P('ep', 'tp'), may hold values from -0.125 to 0.125
- w_fgate: bfloat16 [2048, 8], P('ep', 'tp'), may hold values from -0.125 to 0.125
- igate_bias: float32 [8], P('tp'), may hold values from -2 to 1
- fgate_bias: float32 [8], P('tp'), may hold values from 0 to 4
- head_gain: float32 [512], P('tp'), may hold values from 0.1 to 1.9
- w_out: bfloat16 [512, 2048], P('tp', 'ep'), may hold values from -0.25 to 0.25
- state_matrix: float32 [512, 8, 64, 64], P('ep', 'tp'), may hold values from -2.4 to 2.4
- state_norm: float32 [512, 8, 64], P('ep', 'tp'), may hold values from -2.4 to 2.4
- state_max: float32 [512, 8], P('ep', 'tp'), may hold values from -4 to 4
- ffn_gain: float32 [2048], replicated, may hold values from 0.1 to 1.9
- w_expert_gate: bfloat16 [16, 2048, 1408], P('ep', None, 'tp'), may hold values from -0.125 to 0.125
- w_expert_up: bfloat16 [16, 2048, 1408], P('ep', None, 'tp'), may hold values from -0.125 to 0.125
- w_expert_down: bfloat16 [16, 1408, 2048], P('ep', 'tp'), may hold values from -0.15625 to 0.15625
- routes: int32 [512, 3], P('ep'), may hold values from 0 to 15, all different within a row; in each aligned block of 32 rows (0 to 31, 32 to 63, ...) at most 12 rows name the same one
- route_weights: float32 [512, 3], P('ep'), may hold values from 0.2 to 1
Outputs:
- mixed: bfloat16 [512, 2048], P('ep')
- new_matrix: float32 [512, 8, 64, 64], P('ep', 'tp')
- new_norm: float32 [512, 8, 64], P('ep', 'tp')
- new_max: float32 [512, 8], P('ep', 'tp')
The draws below stay inside these ranges and needn't reach their ends.
Inputs may be any that keep to these rules, and one draw needn't show every extreme that they name: `routes`: each row names 3 different experts. Among the rows of one device, no expert is named by more than 12 rows, a bound that some block reaches.
All inputs are finite; a program needn't handle non-finite values.
Results may differ from the reference program's by a relative error of at most 0.017.
Values may be sent and summed in bfloat16 or wider, within the bound.
A program may use at most 128 MiB of HBM per device.

```python
import math
import jax
import jax.numpy as jnp
import numpy as np
from jax import lax

D = 2048
HEADS = 8
HEAD_SIZE = 64
HW = 512
D_EXP = 1408
TOPK = 3
EXPERTS = 16
SEQ_DEV = 32
B = 512
CAP = 12
N_EP = 16
N_TP = 2


def steps_of(stream_key, shape, split, low, high):
    level = 1.0
    for position, shards_of in split:
        draws = jax.random.uniform(jax.random.fold_in(jax.random.fold_in(stream_key, 6), position), (shards_of,), jnp.float32, low / len(split), high / len(split))
        level = level * jnp.repeat(jnp.exp(draws), shape[position] // shards_of).reshape((-1,) + (1,) * (len(shape) - 1 - position))
    return level


def routed_block(stream_key, own, number, rows, amount, top, reach, lean):
    order = jax.random.permutation(stream_key, amount)
    packed, usual = load_shares(amount, rows * top, reach, lean, True), load_shares(amount, rows * top, reach, lean, False)
    places = jnp.arange(amount)

    def named(tallies, offset_by):
        used = int((tallies > 0).sum())
        fixed = max(1, used // 4)
        shifted = fixed + (places - fixed + offset_by * (used - fixed)) % max(1, amount - fixed)
        return jnp.zeros((amount,), jnp.int32).at[order[jnp.where(places < fixed, places, shifted)]].set(jnp.asarray(tallies, jnp.int32))

    tallies = jnp.where(number % 4 == 0, named(packed, number // 4), named(usual, number - number // 4 - 1))
    mixed = jax.random.permutation(jax.random.fold_in(own, 3), amount)
    source_of, sink = mixed[0:amount // 2 * 2:2], mixed[1:amount // 2 * 2:2]
    room = jnp.minimum(tallies[source_of] - 1, reach - tallies[sink]) // 2
    room = jnp.where((source_of == order[0]) | (sink == order[0]) | (tallies[sink] == 0), 0, jnp.maximum(room, 0))
    shifted = jax.random.randint(jax.random.fold_in(own, 4), (amount // 2,), 0, 1 << 20) % (room + 1)
    tallies = tallies.at[source_of].add(-shifted).at[sink].add(shifted)
    labels = jnp.searchsorted(jnp.cumsum(tallies), jnp.arange(rows * top), side="right").astype(jnp.int32)
    listing = labels.reshape(top, rows).T
    listing = listing[jax.random.permutation(jax.random.fold_in(own, 1), rows)]
    offset_by = jax.random.randint(jax.random.fold_in(own, 2), (rows, 1), 0, top)
    return jnp.take_along_axis(listing, (jnp.arange(top)[None, :] + offset_by) % top, axis=1)


def load_shares(number_of, total, reach, lean, full):
    loads = [(1 << 20) // math.isqrt(rank ** lean) + 1 for rank in range(1, number_of + 1)]
    largest = reach if full else min(reach, max(-(-total // number_of), total * loads[0] // sum(loads)))
    least = 1 if total - largest >= number_of - 1 else 0
    given, rest = [largest] + [least] * (number_of - 1), total - largest - least * (number_of - 1)
    while rest > 0:
        candidates = [i for i in range(1, number_of) if given[i] < largest] or [i for i in range(1, number_of) if given[i] < reach]
        pool, budget = sum([loads[i] for i in candidates]), rest
        for i in candidates:
            more = min(reach - given[i], max(1, budget * loads[i] // pool), rest)
            given[i] = given[i] + more
            rest = rest - more
    return np.array(given)


def normal_values(key, dims, spread, limit, pieces=(), kind=jnp.bfloat16):
    values = jax.random.normal(key, dims, jnp.float32) * spread
    if len(pieces) > 0:
        values = steps_of(key, dims, pieces, -0.22, 0.18) * values
    return jnp.clip(values, min=-limit, max=limit).astype(kind)


def setup_inputs(seed: int = 0) -> dict:
    arg_keys = jax.random.split(jax.random.key(seed), 22)
    tokens = normal_values(arg_keys[0], (B, D), 1.0, 6.0, ((0, 16),))
    mix_gain = jnp.clip(1.0 + 0.18 * jax.random.normal(arg_keys[1], (D,), jnp.float32), 0.1, 1.9)
    w_query = normal_values(arg_keys[2], (D, HW), D ** -0.5, 0.125, ((0, 16), (1, 2)))
    w_key = normal_values(arg_keys[3], (D, HW), D ** -0.5, 0.125, ((0, 16), (1, 2)))
    w_value = normal_values(arg_keys[4], (D, HW), D ** -0.5, 0.125, ((0, 16), (1, 2)))
    w_outgate = normal_values(arg_keys[5], (D, HW), D ** -0.5, 0.125, ((0, 16), (1, 2)))
    w_igate = normal_values(arg_keys[6], (D, HEADS), D ** -0.5, 0.125, ((0, 16), (1, 2)))
    w_fgate = normal_values(arg_keys[7], (D, HEADS), D ** -0.5, 0.125, ((0, 16), (1, 2)))
    igate_bias = jnp.clip(-2.0 + 3.0 * jax.random.uniform(arg_keys[8], (HEADS,), jnp.float32) ** steps_of(arg_keys[8], (HEADS,), ((0, 2),), -0.2, 0.2), -2.0, 1.0)
    fgate_bias = jnp.clip(4.0 * jax.random.uniform(arg_keys[9], (HEADS,), jnp.float32) ** steps_of(arg_keys[9], (HEADS,), ((0, 2),), -0.2, 0.2), 0.0, 4.0)
    head_gain = jnp.clip(1.0 + 0.18 * jax.random.normal(arg_keys[10], (HW,), jnp.float32), 0.1, 1.9)
    w_out = normal_values(arg_keys[11], (HW, D), HW ** -0.5, 0.25, ((0, 2), (1, 16)))
    state_matrix = normal_values(arg_keys[12], (B, HEADS, HEAD_SIZE, HEAD_SIZE), 0.3, 2.4, ((0, 16), (1, 2)), jnp.float32)
    state_norm = normal_values(arg_keys[13], (B, HEADS, HEAD_SIZE), 0.3, 2.4, ((0, 16), (1, 2)), jnp.float32)
    state_max = normal_values(arg_keys[14], (B, HEADS), 1.0, 4.0, ((0, 16), (1, 2)), jnp.float32)
    ffn_gain = jnp.clip(1.0 + 0.18 * jax.random.normal(arg_keys[15], (D,), jnp.float32), 0.1, 1.9)
    w_expert_gate = normal_values(arg_keys[16], (EXPERTS, D, D_EXP), D ** -0.5, 0.125, ((0, 16), (2, 2)))
    w_expert_up = normal_values(arg_keys[17], (EXPERTS, D, D_EXP), D ** -0.5, 0.125, ((0, 16), (2, 2)))
    w_expert_down = normal_values(arg_keys[18], (EXPERTS, D_EXP, D), D_EXP ** -0.5, 0.15625, ((0, 16), (1, 2)))
    routes_keys = jax.random.split(jax.random.fold_in(arg_keys[19], 1), B // SEQ_DEV)
    routes_turns = jax.random.permutation(jax.random.fold_in(arg_keys[19], 3), B // SEQ_DEV)
    routes = jax.vmap(lambda own, number: routed_block(jax.random.fold_in(arg_keys[19], 2), own, number, SEQ_DEV, EXPERTS, TOPK, CAP, 2))(routes_keys, routes_turns).reshape((B, TOPK))
    route_weights = jnp.clip(0.2 + 0.8 * jax.random.uniform(arg_keys[20], (B, TOPK), jnp.float32) ** steps_of(arg_keys[20], (B, TOPK), ((0, 16),), -0.2, 0.2), 0.2, 1.0)
    return {"tokens": tokens, "mix_gain": mix_gain, "w_query": w_query, "w_key": w_key, "w_value": w_value, "w_outgate": w_outgate, "w_igate": w_igate, "w_fgate": w_fgate, "igate_bias": igate_bias, "fgate_bias": fgate_bias, "head_gain": head_gain, "w_out": w_out, "state_matrix": state_matrix, "state_norm": state_norm, "state_max": state_max, "ffn_gain": ffn_gain, "w_expert_gate": w_expert_gate, "w_expert_up": w_expert_up, "w_expert_down": w_expert_down, "routes": routes, "route_weights": route_weights}


def rms_scale(values_in, gain_vec):
    widened = values_in.astype(jnp.float32)
    return widened * lax.rsqrt(lax.optimization_barrier(jnp.mean(widened * widened, axis=-1, keepdims=True)) + 1e-06) * gain_vec

def memory_cell(query, key_row, value_row, outgate, input_pre, forget_pre, head_gain, state_matrix, state_norm, state_max):
    seq_rows, head_count = input_pre.shape
    head_size = query.shape[1] // head_count
    query_heads = query.astype(jnp.float32).reshape(seq_rows, head_count, head_size)
    key_heads = key_row.astype(jnp.float32).reshape(seq_rows, head_count, head_size) * head_size ** (-0.5)
    value_heads = value_row.astype(jnp.float32).reshape(seq_rows, head_count, head_size)
    log_forget = jax.nn.log_sigmoid(forget_pre)
    new_max = jnp.maximum(log_forget + state_max, input_pre)
    keep_old = jnp.exp(log_forget + state_max - new_max)
    keep_new = jnp.exp(input_pre - new_max)
    new_matrix = keep_old[:, :, None, None] * state_matrix + keep_new[:, :, None, None] * value_heads[:, :, :, None] * key_heads[:, :, None, :]
    new_norm = keep_old[:, :, None] * state_norm + keep_new[:, :, None] * key_heads
    numerator = jnp.einsum('bhvd,bhd->bhv', new_matrix, query_heads, precision=lax.Precision.HIGHEST)
    denominator = lax.optimization_barrier(jnp.sum(new_norm * query_heads, axis=-1))
    cell_read = numerator / jnp.maximum(jnp.abs(denominator), jnp.exp(-new_max))[:, :, None]
    centered = cell_read - lax.optimization_barrier(jnp.mean(cell_read, axis=-1, keepdims=True))
    variance = lax.optimization_barrier(jnp.mean(centered * centered, axis=-1, keepdims=True))
    scaled_cell = (centered * lax.rsqrt(variance + 1e-06)).reshape(seq_rows, head_count * head_size)
    cell_out = (scaled_cell * head_gain * jax.nn.sigmoid(outgate.astype(jnp.float32))).astype(jnp.bfloat16)
    return (cell_out, new_matrix, new_norm, new_max)

def reference(tokens, mix_gain, w_query, w_key, w_value, w_outgate, w_igate, w_fgate, igate_bias, fgate_bias, head_gain, w_out, state_matrix, state_norm, state_max, ffn_gain, w_expert_gate, w_expert_up, w_expert_down, routes, route_weights):
    normed = rms_scale(tokens, mix_gain).astype(jnp.bfloat16)

    def project(weight):
        return jnp.dot(normed, weight, preferred_element_type=jnp.float32)
    query = project(w_query).astype(jnp.bfloat16)
    key_row = project(w_key).astype(jnp.bfloat16)
    value_row = project(w_value).astype(jnp.bfloat16)
    outgate = project(w_outgate).astype(jnp.bfloat16)
    input_pre = project(w_igate) + igate_bias
    forget_pre = project(w_fgate) + fgate_bias
    cell_out, new_matrix, new_norm, new_max = memory_cell(query, key_row, value_row, outgate, input_pre, forget_pre, head_gain, state_matrix, state_norm, state_max)
    seq_rows, width = tokens.shape
    cell_width = cell_out.shape[1]
    blocks = jnp.einsum('bth,thd->btd', cell_out.astype(jnp.float32).reshape(seq_rows, N_TP, cell_width // N_TP), w_out.astype(jnp.float32).reshape(N_TP, cell_width // N_TP, width))
    rounded = lax.optimization_barrier(blocks.astype(jnp.bfloat16))
    resid = (tokens.astype(jnp.float32) + lax.optimization_barrier(jnp.sum(rounded.astype(jnp.float32), axis=1))).astype(jnp.bfloat16)
    normed_two = rms_scale(resid, ffn_gain).astype(jnp.bfloat16)
    groups = N_EP
    per_group = seq_rows // groups
    expert_total = w_expert_gate.shape[0]
    top_count = routes.shape[1]
    flat_routes = routes.reshape(groups, per_group * top_count)
    onehot = (flat_routes[:, :, None] == jnp.arange(expert_total, dtype=jnp.int32)[None, None, :]).astype(jnp.int32)
    earlier = jnp.cumsum(onehot, axis=1, dtype=jnp.int32) - onehot
    slots = lax.optimization_barrier(jnp.sum(onehot * earlier, axis=-1, dtype=jnp.int32)).astype(jnp.int32)
    group_ids = jnp.broadcast_to(jnp.arange(groups, dtype=jnp.int32)[:, None], flat_routes.shape)
    token_ids = (jnp.arange(seq_rows * top_count, dtype=jnp.int32) // top_count).reshape(groups, per_group * top_count)
    table = jnp.zeros((expert_total, groups, CAP), jnp.int32).at[flat_routes, group_ids, slots].set(token_ids)

    def run_expert(operands):
        gate_weight, up_weight, down_weight, row_ids = operands
        rows = normed_two[row_ids.reshape(-1)]
        gate_pre = jnp.dot(rows, gate_weight, preferred_element_type=jnp.float32)
        up_pre = jnp.dot(rows, up_weight, preferred_element_type=jnp.float32)
        hidden = (jax.nn.silu(gate_pre) * up_pre).astype(jnp.bfloat16)
        expert_width = hidden.shape[1]
        parts = jnp.einsum('rtf,tfd->rtd', hidden.astype(jnp.float32).reshape(-1, N_TP, expert_width // N_TP), down_weight.astype(jnp.float32).reshape(N_TP, expert_width // N_TP, width))
        rounded_parts = lax.optimization_barrier(parts.astype(jnp.bfloat16))
        return lax.optimization_barrier(jnp.sum(rounded_parts.astype(jnp.float32), axis=1)).astype(jnp.bfloat16)
    outputs = lax.map(run_expert, (w_expert_gate, w_expert_up, w_expert_down, table))
    picked = outputs[flat_routes, group_ids * CAP + slots]
    picked = picked.reshape(seq_rows, top_count, width).astype(jnp.float32)
    mixed = (resid.astype(jnp.float32) + lax.optimization_barrier(jnp.sum(picked * route_weights[:, :, None], axis=1))).astype(jnp.bfloat16)
    return (mixed, new_matrix, new_norm, new_max)
```

```python
import functools

import jax
import jax.numpy as jnp
from jax import lax
from jax.experimental import pallas as pl
from jax.experimental.pallas import tpu as pltpu
from jax.sharding import PartitionSpec as P

MESH = pl.DeviceIdType.MESH
PLANE = 4
LANES = 128
SLOT_TILE = 16
VMEM_BYTES = 60 * 1024 * 1024


def remote(src, dst, send_sem, recv_sem, target):
    return pltpu.make_async_remote_copy(
        src_ref=src,
        dst_ref=dst,
        send_sem=send_sem,
        recv_sem=recv_sem,
        device_id=target,
        device_id_type=MESH,
    )


def dot_t(left, right):
    return lax.dot_general(
        left, right, (((1,), (1,)), ((), ())), preferred_element_type=jnp.float32
    )


def mixer_kernel(
    lines,
    tokens_ref,
    gain_ref,
    wq_ref,
    wk_ref,
    wv_ref,
    wo_gate_ref,
    gates_ref,
    w_out_ref,
    proj_ref,
    w_all_ref,
    normed,
    spread,
    weights,
    partial,
    outgoing,
    arrived,
    local_sem,
    w_send,
    w_recv,
    x_send,
    x_recv,
    p_send,
    p_recv,
    z_send,
    z_recv,
    o_send,
    o_recv,
):
    ep, tp = lax.axis_index("ep"), lax.axis_index("tp")
    line, spot = ep // PLANE, ep % PLANE
    rows, width = tokens_ref.shape
    depth = wq_ref.shape[0]
    block = depth * PLANE

    def line_peer(step):
        other = lax.rem(line + step, lines)
        return other, (other * PLANE + spot, tp)

    def plane_peer(step):
        return (line * PLANE + lax.rem(spot + step, PLANE), tp)

    own_rows = pl.ds(pl.multiple_of(spot * depth, depth), depth)
    copies = []
    start = 0
    for index, ref in enumerate((wq_ref, wk_ref, wv_ref, wo_gate_ref, gates_ref)):
        columns = ref.shape[1]
        copy = pltpu.make_async_copy(
            ref, weights.at[own_rows, start : start + columns], local_sem.at[index]
        )
        copy.start()
        copies.append(copy)
        start += columns
    keep_out = pltpu.make_async_copy(w_out_ref, w_all_ref.at[spot, line], local_sem.at[5])
    keep_out.start()
    barrier = pltpu.get_barrier_semaphore()
    for step in range(1, lines):
        pl.semaphore_signal(barrier, inc=1, device_id=line_peer(step)[1], device_id_type=MESH)
    for step in range(1, PLANE):
        pl.semaphore_signal(barrier, inc=1, device_id=plane_peer(step), device_id_type=MESH)
    widened = tokens_ref[...].astype(jnp.float32)
    scale = lax.rsqrt(jnp.mean(widened * widened, axis=-1, keepdims=True) + 1e-06)
    normed[...] = (widened * scale * gain_ref[...]).astype(jnp.bfloat16)
    pl.semaphore_wait(barrier, lines - 1 + PLANE - 1)
    for copy in copies:
        copy.wait()
    w_copies, x_copies, z_copies, p_copies, o_copies = [], [], [], [], []
    for step in range(1, PLANE):
        copy = remote(
            weights.at[own_rows],
            weights.at[own_rows],
            w_send.at[step],
            w_recv.at[step],
            plane_peer(step),
        )
        copy.start()
        w_copies.append(copy)
    for step in range(1, lines):
        other, target = line_peer(step)
        copy = remote(
            normed.at[:, pl.ds(pl.multiple_of(other * block, block), block)],
            spread.at[line],
            x_send.at[step],
            x_recv.at[step],
            target,
        )
        copy.start()
        x_copies.append(copy)
    for step in range(1, lines):
        copy = remote(
            w_out_ref,
            w_all_ref.at[spot, line],
            z_send.at[step],
            z_recv.at[step],
            line_peer(step)[1],
        )
        copy.start()
        z_copies.append(copy)
    spread[line] = normed[:, pl.ds(pl.multiple_of(line * block, block), block)]
    keep_out.wait()
    for copy in x_copies:
        copy.wait()
    for copy in z_copies:
        copy.wait()
    for step in range(1, PLANE):
        copy = remote(
            w_all_ref.at[spot],
            w_all_ref.at[spot],
            o_send.at[step],
            o_recv.at[step],
            plane_peer(step),
        )
        copy.start()
        o_copies.append(copy)
    for copy in w_copies:
        copy.wait()
    main = weights.shape[1] - LANES
    product = jnp.dot(
        spread[...].reshape(lines * rows, block),
        weights[...],
        preferred_element_type=jnp.float32,
    )
    outgoing[:, :, :main] = product[:, :main].astype(jnp.bfloat16).reshape(lines, rows, main)
    gates = product[:, main:]
    coarse = gates.astype(jnp.bfloat16)
    fine = (gates - coarse.astype(jnp.float32)).astype(jnp.bfloat16)
    first = lax.broadcasted_iota(jnp.int32, gates.shape, 1) < LANES // 2
    picked = jnp.where(first, coarse.astype(jnp.float32), fine.astype(jnp.float32))
    outgoing[:, :, main:] = picked.astype(jnp.bfloat16).reshape(lines, rows, LANES)
    partial[:, :, :main] = product[:, :main].reshape(lines, rows, main)
    partial[:, :, main:] = jnp.where(first, gates, 0.0).reshape(lines, rows, LANES)
    for step in range(1, lines):
        other, target = line_peer(step)
        copy = remote(
            outgoing.at[other], arrived.at[step], p_send.at[step], p_recv.at[step], target
        )
        copy.start()
        p_copies.append(copy)
    total = partial[line]
    for step in range(1, lines):
        p_copies[step - 1].wait()
        total = total + arrived[step].astype(jnp.float32)
    proj_ref[...] = total
    for copy in o_copies:
        copy.wait()


def expert_kernel(
    count,
    cell_ref,
    w_all_ref,
    tokens_ref,
    gain_ref,
    target_rows_ref,
    target_cols_ref,
    route_weights_ref,
    w_gate_hbm,
    w_up_hbm,
    w_down_hbm,
    mixed_ref,
    w_gate,
    w_up,
    w_down,
    mine,
    theirs,
    resid,
    outgoing,
    near,
    far,
    down_send,
    down_recv,
    finished,
    returned,
    last_send,
    last_recv,
    local_sem,
    t_send,
    t_recv,
    d_send,
    d_recv,
    f_send,
    f_recv,
    r_send,
    r_recv,
):
    ep, tp = lax.axis_index("ep"), lax.axis_index("tp")
    partner = (ep, 1 - tp)
    rows, width = tokens_ref.shape
    half = width // 2
    slots = count * SLOT_TILE
    top = route_weights_ref.shape[1]
    loads = []
    for index, (source, kept) in enumerate(
        ((w_gate_hbm, w_gate), (w_up_hbm, w_up), (w_down_hbm, w_down))
    ):
        copy = pltpu.make_async_copy(source, kept, local_sem.at[index])
        copy.start()
        loads.append(copy)
    barrier = pltpu.get_barrier_semaphore()
    for step in range(1, count):
        pl.semaphore_signal(
            barrier, inc=1, device_id=(lax.rem(ep + step, count), tp), device_id_type=MESH
        )
    pl.semaphore_signal(barrier, inc=1, device_id=partner, device_id_type=MESH)
    cell = cell_ref[...]
    columns = w_all_ref.shape[3]
    lines = w_all_ref.shape[1]
    for line in range(lines):
        for spot in range(PLANE):
            start = (line * PLANE + spot) * columns
            mine[:, start : start + columns] = jnp.dot(
                cell, w_all_ref[spot, line], preferred_element_type=jnp.float32
            ).astype(jnp.bfloat16)
    pl.semaphore_wait(barrier, count)
    swap = remote(mine, theirs, t_send.at[0], t_recv.at[0], partner)
    swap.start()
    slot_row = lax.broadcasted_iota(jnp.int32, (slots, rows), 0)
    dispatch = jnp.zeros((slots, rows), jnp.float32)
    for k in range(top):
        dispatch += jnp.where(slot_row == target_rows_ref[k : k + 1, :], 1.0, 0.0)
    dispatch = dispatch.astype(jnp.bfloat16)
    swap.wait()
    summed = mine[...].astype(jnp.float32) + theirs[...].astype(jnp.float32)
    resid[...] = (tokens_ref[...].astype(jnp.float32) + summed).astype(jnp.bfloat16)
    widened = resid[...].astype(jnp.float32)
    scale = lax.rsqrt(jnp.mean(widened * widened, axis=-1, keepdims=True) + 1e-06)
    my_half = pl.ds(pl.multiple_of(tp * half, half), half)
    other_half = pl.ds(pl.multiple_of((1 - tp) * half, half), half)
    normed = (resid[:, my_half].astype(jnp.float32) * scale * gain_ref[:, my_half]).astype(
        jnp.bfloat16
    )
    outgoing[...] = (
        jnp.dot(dispatch, normed, preferred_element_type=jnp.float32)
        .astype(jnp.bfloat16)
        .reshape(count, SLOT_TILE, half)
    )
    sends = []
    for step in range(1, count):
        other = lax.rem(ep + step, count)
        copy = remote(
            outgoing.at[other], near.at[ep], d_send.at[step], d_recv.at[step], (other, tp)
        )
        copy.start()
        sends.append(copy)
    near[ep] = outgoing[ep]
    forwards = []
    for step in range(count):
        source = lax.rem(ep + count - step, count)
        if step > 0:
            sends[step - 1].wait()
        copy = remote(
            near.at[source] if step > 0 else outgoing.at[ep],
            far.at[source],
            f_send.at[step],
            f_recv.at[step],
            partner,
        )
        copy.start()
        forwards.append(copy)
    for copy in loads:
        copy.wait()
    near_rows = near[...].reshape(slots, half)
    gate_pre = dot_t(near_rows, w_gate[:, my_half])
    up_pre = dot_t(near_rows, w_up[:, my_half])
    for copy in forwards:
        copy.wait()
    far_rows = far[...].reshape(slots, half)
    gate_pre += dot_t(far_rows, w_gate[:, other_half])
    up_pre += dot_t(far_rows, w_up[:, other_half])
    hidden = (gate_pre * jax.nn.sigmoid(gate_pre) * up_pre).astype(jnp.bfloat16)
    down_send[...] = jnp.dot(
        hidden, w_down[:, other_half], preferred_element_type=jnp.float32
    ).astype(jnp.bfloat16)
    swap = remote(down_send, down_recv, t_send.at[1], t_recv.at[1], partner)
    swap.start()
    kept = jnp.dot(hidden, w_down[:, my_half], preferred_element_type=jnp.float32).astype(
        jnp.bfloat16
    )
    swap.wait()
    finished[...] = (
        (kept.astype(jnp.float32) + down_recv[...].astype(jnp.float32))
        .astype(jnp.bfloat16)
        .reshape(count, SLOT_TILE, half)
    )
    sends = []
    for step in range(1, count):
        other = lax.rem(ep + step, count)
        copy = remote(
            finished.at[other], returned.at[ep], r_send.at[step], r_recv.at[step], (other, tp)
        )
        copy.start()
        sends.append(copy)
    returned[ep] = finished[ep]
    slot_col = lax.broadcasted_iota(jnp.int32, (rows, slots), 1)
    combine = jnp.zeros((rows, slots), jnp.float32)
    for k in range(top):
        combine += jnp.where(
            slot_col == target_cols_ref[:, k : k + 1], route_weights_ref[:, k : k + 1], 0.0
        )
    coarse = combine.astype(jnp.bfloat16)
    fine = (combine - coarse.astype(jnp.float32)).astype(jnp.bfloat16)
    for copy in sends:
        copy.wait()
    back = returned[...].reshape(slots, half)
    weighted = jnp.dot(coarse, back, preferred_element_type=jnp.float32) + jnp.dot(
        fine, back, preferred_element_type=jnp.float32
    )
    last_send[...] = (resid[:, my_half].astype(jnp.float32) + weighted).astype(jnp.bfloat16)
    swap = remote(last_send, last_recv, t_send.at[2], t_recv.at[2], partner)
    swap.start()
    mixed_ref[:, my_half] = last_send[...]
    swap.wait()
    mixed_ref[:, other_half] = last_recv[...]


def mixer_call(tokens, mix_gain, weight_list, w_out):
    rows, width = tokens.shape
    w_query, w_key, w_value, w_outgate, w_igate, w_fgate = weight_list
    depth, columns = w_query.shape
    lines = lax.axis_size("ep") // PLANE
    heads = w_igate.shape[1]
    pair = jnp.concatenate((w_igate, w_fgate), axis=1)
    pad = jnp.zeros((depth, LANES // 2 - 2 * heads), pair.dtype)
    gates = jnp.concatenate((pair, pad, pair, pad), axis=1)
    total = 4 * columns + LANES
    vmem = pl.BlockSpec(memory_space=pltpu.VMEM)
    anywhere = pl.BlockSpec(memory_space=pl.ANY)
    dma = pltpu.SemaphoreType.DMA
    proj, w_all = pl.pallas_call(
        functools.partial(mixer_kernel, lines),
        out_shape=(
            jax.ShapeDtypeStruct((rows, total), jnp.float32),
            jax.ShapeDtypeStruct((PLANE, lines) + w_out.shape, jnp.bfloat16),
        ),
        in_specs=[vmem, vmem] + [anywhere] * 5 + [vmem],
        out_specs=(vmem, anywhere),
        scratch_shapes=[
            pltpu.VMEM((rows, width), jnp.bfloat16),
            pltpu.VMEM((lines, rows, depth * PLANE), jnp.bfloat16),
            pltpu.VMEM((depth * PLANE, total), jnp.bfloat16),
            pltpu.VMEM((lines, rows, total), jnp.float32),
            pltpu.VMEM((lines, rows, total), jnp.bfloat16),
            pltpu.VMEM((lines, rows, total), jnp.bfloat16),
            dma((6,)),
            dma((PLANE,)),
            dma((PLANE,)),
            dma((lines,)),
            dma((lines,)),
            dma((lines,)),
            dma((lines,)),
            dma((lines,)),
            dma((lines,)),
            dma((PLANE,)),
            dma((PLANE,)),
        ],
        compiler_params=pltpu.CompilerParams(
            collective_id=0, has_side_effects=True, vmem_limit_bytes=16 * 1024 * 1024
        ),
    )(tokens, mix_gain[None, :], w_query, w_key, w_value, w_outgate, gates, w_out)
    main = 4 * columns
    gate_sums = proj[:, main : main + LANES // 2] + proj[:, main + LANES // 2 :]
    return (
        proj[:, :columns],
        proj[:, columns : 2 * columns],
        proj[:, 2 * columns : 3 * columns],
        proj[:, 3 * columns : main],
        gate_sums[:, :heads],
        gate_sums[:, heads : 2 * heads],
    ), w_all


def expert_call(
    cell_out, w_all, tokens, ffn_gain, routes, route_weights, w_gate, w_up, w_down
):
    rows, width = tokens.shape
    count = lax.axis_size("ep")
    flat = routes.reshape(-1)
    same = (flat[:, None] == flat[None, :]).astype(jnp.int32)
    order = jnp.arange(flat.shape[0], dtype=jnp.int32)
    earlier = (order[None, :] < order[:, None]).astype(jnp.int32)
    slots = jnp.sum(same * earlier, axis=1, dtype=jnp.int32)
    targets = (flat * SLOT_TILE + slots).reshape(routes.shape)
    gate_t = jnp.swapaxes(w_gate[0], 0, 1)
    up_t = jnp.swapaxes(w_up[0], 0, 1)
    down = w_down[0]
    half = width // 2
    area = count * SLOT_TILE
    vmem = pl.BlockSpec(memory_space=pltpu.VMEM)
    anywhere = pl.BlockSpec(memory_space=pl.ANY)
    dma = pltpu.SemaphoreType.DMA
    bf = jnp.bfloat16
    tile = (count, SLOT_TILE, half)
    return pl.pallas_call(
        functools.partial(expert_kernel, count),
        out_shape=jax.ShapeDtypeStruct((rows, width), bf),
        in_specs=[vmem] * 7 + [anywhere] * 3,
        out_specs=vmem,
        scratch_shapes=[
            pltpu.VMEM(gate_t.shape, bf),
            pltpu.VMEM(up_t.shape, bf),
            pltpu.VMEM(down.shape, bf),
            pltpu.VMEM((rows, width), bf),
            pltpu.VMEM((rows, width), bf),
            pltpu.VMEM((rows, width), bf),
            pltpu.VMEM(tile, bf),
            pltpu.VMEM(tile, bf),
            pltpu.VMEM(tile, bf),
            pltpu.VMEM((area, half), bf),
            pltpu.VMEM((area, half), bf),
            pltpu.VMEM(tile, bf),
            pltpu.VMEM(tile, bf),
            pltpu.VMEM((rows, half), bf),
            pltpu.VMEM((rows, half), bf),
            dma((3,)),
            dma((3,)),
            dma((3,)),
            dma((count,)),
            dma((count,)),
            dma((count,)),
            dma((count,)),
            dma((count,)),
            dma((count,)),
        ],
        compiler_params=pltpu.CompilerParams(
            collective_id=1, has_side_effects=True, vmem_limit_bytes=40 * 1024 * 1024
        ),
    )(
        cell_out,
        w_all,
        tokens,
        ffn_gain[None, :],
        jnp.swapaxes(targets, 0, 1),
        targets,
        route_weights,
        gate_t,
        up_t,
        down,
    )


def rms_scale(values_in, gain_vec):
    widened = values_in.astype(jnp.float32)
    return (
        widened * lax.rsqrt(jnp.mean(widened * widened, axis=-1, keepdims=True) + 1e-06) * gain_vec
    )


def memory_cell(
    query,
    key_row,
    value_row,
    outgate,
    input_pre,
    forget_pre,
    head_gain,
    state_matrix,
    state_norm,
    state_max,
):
    seq_rows, head_count = input_pre.shape
    head_size = query.shape[1] // head_count
    query_heads = query.astype(jnp.float32).reshape(seq_rows, head_count, head_size)
    key_heads = key_row.astype(jnp.float32).reshape(
        seq_rows, head_count, head_size
    ) * head_size ** (-0.5)
    value_heads = value_row.astype(jnp.float32).reshape(seq_rows, head_count, head_size)
    log_forget = jax.nn.log_sigmoid(forget_pre)
    new_max = jnp.maximum(log_forget + state_max, input_pre)
    keep_old = jnp.exp(log_forget + state_max - new_max)
    keep_new = jnp.exp(input_pre - new_max)
    new_matrix = (
        keep_old[:, :, None, None] * state_matrix
        + keep_new[:, :, None, None] * value_heads[:, :, :, None] * key_heads[:, :, None, :]
    )
    new_norm = keep_old[:, :, None] * state_norm + keep_new[:, :, None] * key_heads
    numerator = jnp.einsum(
        "bhvd,bhd->bhv", new_matrix, query_heads, precision=lax.Precision.HIGHEST
    )
    denominator = jnp.sum(new_norm * query_heads, axis=-1)
    cell_read = numerator / jnp.maximum(jnp.abs(denominator), jnp.exp(-new_max))[:, :, None]
    centered = cell_read - jnp.mean(cell_read, axis=-1, keepdims=True)
    variance = jnp.mean(centered * centered, axis=-1, keepdims=True)
    scaled_cell = (centered * lax.rsqrt(variance + 1e-06)).reshape(seq_rows, head_count * head_size)
    cell_out = (scaled_cell * head_gain * jax.nn.sigmoid(outgate.astype(jnp.float32))).astype(
        jnp.bfloat16
    )
    return (cell_out, new_matrix, new_norm, new_max)


def kernels_fit(tokens, w_query, w_igate, w_out, w_expert_gate, routes):
    ep_count = lax.axis_size("ep")
    rows, width = tokens.shape
    capacity = max(2, 2 * rows * routes.shape[1] // (w_expert_gate.shape[0] * ep_count))
    return (
        lax.axis_size("tp") == 2
        and ep_count % PLANE == 0
        and w_query.shape[0] % LANES == 0
        and w_query.shape[1] % LANES == 0
        and w_out.shape[1] % LANES == 0
        and width % (2 * LANES) == 0
        and rows % SLOT_TILE == 0
        and w_igate.shape[1] * 4 <= LANES
        and w_expert_gate.shape[0] == 1
        and capacity <= SLOT_TILE
    )


def body(
    tokens,
    mix_gain,
    w_query,
    w_key,
    w_value,
    w_outgate,
    w_igate,
    w_fgate,
    igate_bias,
    fgate_bias,
    head_gain,
    w_out,
    state_matrix,
    state_norm,
    state_max,
    ffn_gain,
    w_expert_gate,
    w_expert_up,
    w_expert_down,
    routes,
    route_weights,
):
    seq_rows, width = tokens.shape
    weight_list = (w_query, w_key, w_value, w_outgate, w_igate, w_fgate)
    if kernels_fit(tokens, w_query, w_igate, w_out, w_expert_gate, routes):
        projected, w_all = mixer_call(tokens, mix_gain, weight_list, w_out)
        cell_out, new_matrix, new_norm, new_max = memory_cell(
            projected[0].astype(jnp.bfloat16),
            projected[1].astype(jnp.bfloat16),
            projected[2].astype(jnp.bfloat16),
            projected[3].astype(jnp.bfloat16),
            projected[4] + igate_bias,
            projected[5] + fgate_bias,
            head_gain,
            state_matrix,
            state_norm,
            state_max,
        )
        mixed = expert_call(
            cell_out,
            w_all,
            tokens,
            ffn_gain,
            routes,
            route_weights,
            w_expert_gate,
            w_expert_up,
            w_expert_down,
        )
        return (mixed, new_matrix, new_norm, new_max)
    normed = rms_scale(tokens, mix_gain).astype(jnp.bfloat16)
    spread = lax.all_to_all(normed, "ep", split_axis=1, concat_axis=0, tiled=True)
    joined = jnp.concatenate(weight_list, axis=1)
    summed = lax.psum_scatter(
        jnp.dot(spread, joined, preferred_element_type=jnp.float32),
        "ep",
        scatter_dimension=0,
        tiled=True,
    )
    bounds = [0]
    for weight in weight_list:
        bounds.append(bounds[-1] + weight.shape[1])
    projected = tuple(
        (summed[:, bounds[index] : bounds[index + 1]] for index in range(len(weight_list)))
    )
    query = projected[0].astype(jnp.bfloat16)
    key_row = projected[1].astype(jnp.bfloat16)
    value_row = projected[2].astype(jnp.bfloat16)
    outgate = projected[3].astype(jnp.bfloat16)
    input_pre = projected[4] + igate_bias
    forget_pre = projected[5] + fgate_bias
    cell_out, new_matrix, new_norm, new_max = memory_cell(
        query,
        key_row,
        value_row,
        outgate,
        input_pre,
        forget_pre,
        head_gain,
        state_matrix,
        state_norm,
        state_max,
    )
    partial_out = jnp.dot(
        cell_out,
        lax.all_gather(w_out, "ep", axis=1, tiled=True),
        preferred_element_type=jnp.float32,
    )
    attended = lax.psum(partial_out.astype(jnp.bfloat16), "tp").astype(jnp.float32)
    resid = (tokens.astype(jnp.float32) + attended).astype(jnp.bfloat16)
    normed_two = rms_scale(resid, ffn_gain).astype(jnp.bfloat16)
    ep_count = lax.axis_size("ep")
    local_experts = w_expert_gate.shape[0]
    expert_total = local_experts * ep_count
    top_count = routes.shape[1]
    capacity = max(2, 2 * seq_rows * top_count // expert_total)
    flat_routes = routes.reshape(-1)
    onehot = (flat_routes[:, None] == jnp.arange(expert_total, dtype=jnp.int32)[None, :]).astype(
        jnp.int32
    )
    earlier = jnp.cumsum(onehot, axis=0, dtype=jnp.int32) - onehot
    slots = jnp.sum(onehot * earlier, axis=1, dtype=jnp.int32)
    targets = flat_routes * capacity + slots
    dispatch = (
        targets[:, None] == jnp.arange(expert_total * capacity, dtype=jnp.int32)[None, :]
    ).astype(jnp.bfloat16)
    route_rows = jnp.repeat(normed_two, top_count, axis=0)
    outgoing = jnp.einsum(
        "rs,rd->sd", dispatch, route_rows, preferred_element_type=jnp.float32
    ).astype(jnp.bfloat16)
    outgoing = outgoing.reshape(expert_total, capacity, width)
    received = lax.all_to_all(outgoing, "ep", split_axis=0, concat_axis=0, tiled=True)
    slot_count = received.shape[1]
    regrouped = received.reshape(ep_count, local_experts, slot_count, width)
    gate_pre = jnp.einsum(
        "nxcd,xdf->nxcf", regrouped, w_expert_gate, preferred_element_type=jnp.float32
    )
    up_pre = jnp.einsum(
        "nxcd,xdf->nxcf", regrouped, w_expert_up, preferred_element_type=jnp.float32
    )
    hidden = (jax.nn.silu(gate_pre) * up_pre).astype(jnp.bfloat16)
    partial_down = jnp.einsum(
        "nxcf,xfd->nxcd", hidden, w_expert_down, preferred_element_type=jnp.float32
    )
    expert_sum = lax.psum(partial_down.astype(jnp.bfloat16), "tp")
    finished = expert_sum.reshape(ep_count * local_experts, slot_count, width)
    returned = lax.all_to_all(finished, "ep", split_axis=0, concat_axis=0, tiled=True)
    picked = jnp.dot(
        dispatch,
        returned.reshape(expert_total * capacity, width),
        preferred_element_type=jnp.float32,
    )
    weighted = jnp.sum(
        picked.reshape(seq_rows, top_count, width) * route_weights[:, :, None], axis=1
    )
    mixed = (resid.astype(jnp.float32) + weighted).astype(jnp.bfloat16)
    return (mixed, new_matrix, new_norm, new_max)


def solution(mesh):
    placed = (
        P("ep", None),
        P(),
        P("ep", "tp"),
        P("ep", "tp"),
        P("ep", "tp"),
        P("ep", "tp"),
        P("ep", "tp"),
        P("ep", "tp"),
        P("tp"),
        P("tp"),
        P("tp"),
        P("tp", "ep"),
        P("ep", "tp", None, None),
        P("ep", "tp", None),
        P("ep", "tp"),
        P(),
        P("ep", None, "tp"),
        P("ep", None, "tp"),
        P("ep", "tp", None),
        P("ep", None),
        P("ep", None),
    )
    return jax.shard_map(
        body,
        mesh=mesh,
        in_specs=placed,
        out_specs=(P("ep", None), P("ep", "tp", None, None), P("ep", "tp", None), P("ep", "tp")),
        check_vma=False,
    )
```

```python
import functools

import jax
import jax.numpy as jnp
from jax import lax
from jax.experimental import pallas as pl
from jax.experimental.pallas import tpu as pltpu
from jax.sharding import PartitionSpec as P

MESH = pl.DeviceIdType.MESH
PLANE = 4
LANES = 128
SLOT_TILE = 16
VMEM_BYTES = 60 * 1024 * 1024


def remote(src, dst, send_sem, recv_sem, target):
    return pltpu.make_async_remote_copy(
        src_ref=src,
        dst_ref=dst,
        send_sem=send_sem,
        recv_sem=recv_sem,
        device_id=target,
        device_id_type=MESH,
    )


def dot_t(left, right):
    return lax.dot_general(
        left, right, (((1,), (1,)), ((), ())), preferred_element_type=jnp.float32
    )


def fetch_all(pairs, sems):
    copies = []
    for index, (source, kept) in enumerate(pairs):
        copy = pltpu.make_async_copy(source, kept, sems.at[index])
        copy.start()
        copies.append(copy)
    return copies


def mixer_kernel(
    lines,
    tokens_hbm,
    gain_hbm,
    wq_ref,
    wk_ref,
    wv_ref,
    wo_gate_ref,
    igate_hbm,
    fgate_hbm,
    w_out_hbm,
    proj_ref,
    w_all_ref,
    tokens_ref,
    gain_ref,
    igate_ref,
    fgate_ref,
    turned,
    w_planes,
    normed,
    spread,
    weights,
    partial,
    outgoing,
    arrived,
    local_sem,
    w_send,
    w_recv,
    x_send,
    x_recv,
    p_send,
    p_recv,
    z_send,
    z_recv,
    o_send,
    o_recv,
):
    ep, tp = lax.axis_index("ep"), lax.axis_index("tp")
    line, spot = ep // PLANE, ep % PLANE
    rows, width = tokens_ref.shape
    depth = wq_ref.shape[0]
    block = depth * PLANE
    heads = igate_ref.shape[0]
    beside = spot + 1 - 2 * (spot % 2)
    across = lax.rem(spot + 2, PLANE)
    beside_peer = (line * PLANE + beside, tp)
    across_peer = (line * PLANE + across, tp)

    def line_peer(step):
        other = lax.rem(line + step, lines)
        return other, (other * PLANE + spot, tp)

    own_rows = pl.ds(pl.multiple_of(spot * depth, depth), depth)
    pairs = [
        (tokens_hbm, tokens_ref),
        (gain_hbm, gain_ref),
        (igate_hbm, igate_ref),
        (fgate_hbm, fgate_ref),
        (w_out_hbm, w_planes.at[spot, line]),
    ]
    start = 0
    for ref in (wq_ref, wk_ref, wv_ref, wo_gate_ref):
        columns = ref.shape[1]
        pairs.append((ref, weights.at[own_rows, start : start + columns]))
        start += columns
    main = start
    copies = fetch_all(pairs, local_sem)
    barrier = pltpu.get_barrier_semaphore()
    for step in range(1, lines):
        pl.semaphore_signal(barrier, inc=1, device_id=line_peer(step)[1], device_id_type=MESH)
    pl.semaphore_signal(barrier, inc=1, device_id=beside_peer, device_id_type=MESH)
    pl.semaphore_signal(barrier, inc=1, device_id=across_peer, device_id_type=MESH)
    turned[...] = jnp.zeros_like(turned)
    for copy in copies:
        copy.wait()
    for place in (0, LANES // 2):
        turned[place : place + heads, :] = igate_ref[...].astype(jnp.float32)
        turned[place + heads : place + 2 * heads, :] = fgate_ref[...].astype(jnp.float32)
    weights[own_rows, main:] = turned[...].T.astype(jnp.bfloat16)
    widened = tokens_ref[...].astype(jnp.float32)
    scale = lax.rsqrt(jnp.mean(widened * widened, axis=-1, keepdims=True) + 1e-06)
    normed[...] = (widened * scale * gain_ref[...]).astype(jnp.bfloat16)
    pl.semaphore_wait(barrier, lines - 1 + 2)

    def row_part(owner, part):
        size = depth // 2
        return pl.ds(pl.multiple_of(owner * depth + part * size, size), size)

    def w_copy(owner, part, slot, target):
        view = weights.at[row_part(owner, part)]
        return remote(view, view, w_send.at[slot], w_recv.at[slot], target)

    def o_copy(owner, part, slot, target):
        size = lines // 2
        view = w_planes.at[owner, part * size : part * size + size]
        return remote(view, view, o_send.at[slot], o_recv.at[slot], target)

    def open_plane(make):
        first = [
            make(spot, 0, 0, beside_peer),
            make(spot, 1, 2, across_peer),
            make(spot, 1, 1, beside_peer),
            make(spot, 0, 3, across_peer),
        ]
        for copy in first:
            copy.start()
        return first

    def relay_plane(make, first):
        first[0].wait_recv()
        ahead = make(beside, 0, 4, across_peer)
        ahead.start()
        first[1].wait_recv()
        aside = make(across, 1, 5, beside_peer)
        aside.start()
        return [ahead, aside]

    def close_plane(first, second):
        first[2].wait_recv()
        first[3].wait_recv()
        for copy in first:
            copy.wait_send()
        for copy in second:
            copy.wait()

    w_first = open_plane(w_copy)
    x_copies, z_copies, p_copies = [], [], []
    for step in range(1, lines):
        other, target = line_peer(step)
        copy = remote(
            normed.at[:, pl.ds(pl.multiple_of(other * block, block), block)],
            spread.at[line],
            x_send.at[step],
            x_recv.at[step],
            target,
        )
        copy.start()
        x_copies.append(copy)
    for step in range(1, lines):
        own = w_planes.at[spot, line]
        copy = remote(own, own, z_send.at[step], z_recv.at[step], line_peer(step)[1])
        copy.start()
        z_copies.append(copy)
    spread[line] = normed[:, pl.ds(pl.multiple_of(line * block, block), block)]
    w_second = relay_plane(w_copy, w_first)
    for copy in z_copies:
        copy.wait()
    o_first = open_plane(o_copy)
    for copy in x_copies:
        copy.wait()
    close_plane(w_first, w_second)
    product = jnp.dot(
        spread[...].reshape(lines * rows, block),
        weights[...],
        preferred_element_type=jnp.float32,
    )
    outgoing[:, :, :main] = product[:, :main].astype(jnp.bfloat16).reshape(lines, rows, main)
    gates = product[:, main:]
    coarse = gates.astype(jnp.bfloat16)
    fine = (gates - coarse.astype(jnp.float32)).astype(jnp.bfloat16)
    first = lax.broadcasted_iota(jnp.int32, gates.shape, 1) < LANES // 2
    picked = jnp.where(first, coarse.astype(jnp.float32), fine.astype(jnp.float32))
    outgoing[:, :, main:] = picked.astype(jnp.bfloat16).reshape(lines, rows, LANES)
    partial[:, :, :main] = product[:, :main].reshape(lines, rows, main)
    partial[:, :, main:] = jnp.where(first, gates, 0.0).reshape(lines, rows, LANES)
    for step in range(1, lines):
        other, target = line_peer(step)
        copy = remote(
            outgoing.at[other], arrived.at[step], p_send.at[step], p_recv.at[step], target
        )
        copy.start()
        p_copies.append(copy)
    o_second = relay_plane(o_copy, o_first)
    total = partial[line]
    for step in range(1, lines):
        p_copies[step - 1].wait()
        total = total + arrived[step].astype(jnp.float32)
    proj_ref[...] = total
    close_plane(o_first, o_second)
    store = pltpu.make_async_copy(w_planes, w_all_ref, local_sem.at[0])
    store.start()
    store.wait()


def cell_kernel(
    proj_ref,
    ibias_hbm,
    fbias_hbm,
    head_gain_hbm,
    matrix_hbm,
    norm_hbm,
    max_hbm,
    cell_ref,
    new_matrix_ref,
    new_norm_ref,
    new_max_ref,
    ibias_ref,
    fbias_ref,
    head_gain_ref,
    matrix,
    state_norm,
    state_max,
    turned,
    decay,
    left,
    keys,
    queries,
    reads,
    sems,
    in_sems,
    out_sems,
):
    rows, heads, size, _ = matrix.shape
    wide = heads * size
    pack = 2 * heads
    chunk = 8
    chunks = rows // chunk
    loads = []
    for index in range(chunks):
        part = pl.ds(index * chunk, chunk)
        copy = pltpu.make_async_copy(matrix_hbm.at[part], matrix.at[part], in_sems.at[index])
        copy.start()
        loads.append(copy)
    small = fetch_all(
        (
            (ibias_hbm, ibias_ref),
            (fbias_hbm, fbias_ref),
            (head_gain_hbm, head_gain_ref),
            (norm_hbm, state_norm),
            (max_hbm, state_max),
        ),
        sems,
    )
    turned[...] = jnp.zeros_like(turned)
    gates = proj_ref[:, 4 * wide :]
    gates = gates + pltpu.roll(gates, LANES // 2, 1)
    forget = pltpu.roll(gates, LANES - heads, 1)
    for copy in small:
        copy.wait()
    turned[:heads, :rows] = state_max[...]
    old_max = turned[...].T[:rows]
    turned[...] = jnp.zeros_like(turned)
    turned[0:1, :heads] = ibias_ref[...]
    turned[1:2, :heads] = fbias_ref[...]
    input_pre = gates + turned[0:1, :]
    forget_pre = forget + turned[1:2, :]
    log_forget = jnp.minimum(forget_pre, 0.0) - jnp.log(1.0 + jnp.exp(-jnp.abs(forget_pre)))
    new_max = jnp.maximum(log_forget + old_max, input_pre)
    keep_old = jnp.exp(log_forget + old_max - new_max)
    keep_new = jnp.exp(input_pre - new_max)
    turned[:rows, :] = new_max
    new_max_ref[...] = turned[...].T[:heads, :rows]
    place = lax.broadcasted_iota(jnp.int32, (rows, pack, LANES), 1)
    lane = lax.broadcasted_iota(jnp.int32, (rows, pack, LANES), 2)
    chosen = (place == lane) | (place == lane + heads)

    def per_head(values):
        spread = jnp.broadcast_to(values[:, None, :], (rows, pack, LANES))
        return jnp.sum(
            jnp.where(chosen & (lane < heads), spread, 0.0), axis=-1, keepdims=True
        )

    old_scale = per_head(keep_old)
    new_scale = per_head(keep_new)
    floor = per_head(jnp.exp(-new_max))
    decay[...] = jnp.broadcast_to(old_scale, decay.shape)
    row = lax.broadcasted_iota(jnp.int32, (rows, pack, wide), 1)
    head = lax.broadcasted_iota(jnp.int32, (rows, pack, wide), 2) // size
    same = (row == head) | (row == head + heads)
    fold = (
        lax.broadcasted_iota(jnp.int32, (wide, size), 0) % size
        == lax.broadcasted_iota(jnp.int32, (wide, size), 1)
    ).astype(jnp.float32).astype(jnp.bfloat16)

    def rounded(index):
        return proj_ref[:, index * wide : (index + 1) * wide].astype(jnp.bfloat16).astype(jnp.float32)

    def split_heads(values):
        spread = jnp.broadcast_to(values[:, None, :], (rows, pack, wide))
        masked = jnp.where(same, spread, 0.0).reshape(rows * pack, wide).astype(jnp.bfloat16)
        return jnp.dot(masked, fold, preferred_element_type=jnp.float32).reshape(
            rows, pack, size
        )

    query = split_heads(rounded(0))
    key = split_heads(rounded(1)) * size ** (-0.5)
    value = jnp.broadcast_to(rounded(2)[:, None, :], (rows, pack, wide))
    value = jnp.where(same, value * new_scale, 0.0)
    coarse = value.astype(jnp.bfloat16).astype(jnp.float32)
    left[...] = jnp.where(row < heads, coarse, value - coarse)
    keys[...] = key
    queries[...] = query
    new_norm = old_scale[:, :heads] * state_norm[...] + (new_scale * key)[:, :heads]
    new_norm_ref[...] = new_norm
    divisor = jnp.sum(new_norm * query[:, :heads], axis=-1, keepdims=True)
    divisor = jnp.maximum(jnp.abs(divisor), floor[:, :heads])
    stores = []
    for index in range(chunks):
        loads[index].wait()

        @pl.loop(0, chunk // 4)
        def _(group):
            for inner in range(4):
                item = index * chunk + group * 4 + inner
                outer = lax.dot_general(
                    left[item].astype(jnp.bfloat16),
                    keys[item].astype(jnp.bfloat16),
                    (((0,), (0,)), ((), ())),
                    preferred_element_type=jnp.float32,
                ).reshape(heads, size, size)
                scale = decay[item][:heads][:, None, :]
                fresh = scale * matrix[item] + outer
                matrix[item] = fresh
                flat = fresh.reshape(wide, size)
                high = flat.astype(jnp.bfloat16)
                low = (flat - high.astype(jnp.float32)).astype(jnp.bfloat16)
                asked = queries[item].astype(jnp.bfloat16)
                reads[item] = dot_t(asked, high) + dot_t(asked, low)

        part = pl.ds(index * chunk, chunk)
        copy = pltpu.make_async_copy(matrix.at[part], new_matrix_ref.at[part], out_sems.at[index])
        copy.start()
        stores.append(copy)
    only = (row == head)[:, :heads]
    read = jnp.where(only, reads[:, :heads, :] / divisor, 0.0)
    mean = jnp.sum(read, axis=-1, keepdims=True) / size
    centered = jnp.where(only, read - mean, 0.0)
    variance = jnp.sum(centered * centered, axis=-1, keepdims=True) / size
    scaled = jnp.sum(centered * lax.rsqrt(variance + 1e-06), axis=1)
    cell_ref[...] = (scaled * head_gain_ref[...] * jax.nn.sigmoid(rounded(3))).astype(jnp.bfloat16)
    for copy in stores:
        copy.wait()


def expert_kernel(
    count,
    cell_hbm,
    w_all_hbm,
    tokens_hbm,
    gain_hbm,
    routes_hbm,
    route_weights_hbm,
    w_gate_hbm,
    w_up_hbm,
    w_down_hbm,
    mixed_ref,
    cell_ref,
    w_all_ref,
    tokens_ref,
    gain_ref,
    routes_ref,
    route_weights_ref,
    w_gate,
    w_up,
    w_down,
    mine,
    theirs,
    resid,
    outgoing,
    near,
    far,
    down_send,
    down_recv,
    finished,
    returned,
    last_send,
    last_recv,
    local_sem,
    t_send,
    t_recv,
    d_send,
    d_recv,
    f_send,
    f_recv,
    r_send,
    r_recv,
):
    ep, tp = lax.axis_index("ep"), lax.axis_index("tp")
    partner = (ep, 1 - tp)
    rows, width = tokens_ref.shape
    half = width // 2
    slots = count * SLOT_TILE
    top = route_weights_ref.shape[0]
    loads = fetch_all(
        (
            (cell_hbm, cell_ref),
            (w_all_hbm, w_all_ref),
            (tokens_hbm, tokens_ref),
            (gain_hbm, gain_ref),
            (routes_hbm, routes_ref),
            (route_weights_hbm, route_weights_ref),
            (w_gate_hbm, w_gate),
            (w_up_hbm, w_up),
            (w_down_hbm, w_down),
        ),
        local_sem,
    )
    barrier = pltpu.get_barrier_semaphore()
    for step in range(1, count):
        pl.semaphore_signal(
            barrier, inc=1, device_id=(lax.rem(ep + step, count), tp), device_id_type=MESH
        )
    pl.semaphore_signal(barrier, inc=1, device_id=partner, device_id_type=MESH)
    for copy in loads[:6]:
        copy.wait()
    loads = loads[6:]
    cell = cell_ref[...]
    columns = w_all_ref.shape[3]
    lines = w_all_ref.shape[1]
    for line in range(lines):
        for spot in range(PLANE):
            start = (line * PLANE + spot) * columns
            mine[:, start : start + columns] = jnp.dot(
                cell, w_all_ref[spot, line], preferred_element_type=jnp.float32
            ).astype(jnp.bfloat16)
    pl.semaphore_wait(barrier, count)
    swap = remote(mine, theirs, t_send.at[0], t_recv.at[0], partner)
    swap.start()
    slot_row = lax.broadcasted_iota(jnp.int32, (slots, rows), 0).astype(jnp.float32)
    expert = lax.broadcasted_iota(jnp.int32, (count, rows), 0).astype(jnp.float32)
    before = (
        lax.broadcasted_iota(jnp.int32, (rows, rows), 0)
        < lax.broadcasted_iota(jnp.int32, (rows, rows), 1)
    ).astype(jnp.float32)
    taken = jnp.zeros((count, 1), jnp.float32)
    dispatch = jnp.zeros((slots, rows), jnp.float32)
    combine = jnp.zeros((slots, rows), jnp.float32)
    for k in range(top):
        named = routes_ref[k : k + 1, :].astype(jnp.float32)
        match = jnp.where(expert == named, 1.0, 0.0)
        earlier = jnp.dot(match, before, preferred_element_type=jnp.float32) + taken
        taken = taken + jnp.sum(match, axis=1, keepdims=True)
        target = named * SLOT_TILE + jnp.sum(match * earlier, axis=0, keepdims=True)
        hit = slot_row == target
        dispatch += jnp.where(hit, 1.0, 0.0)
        combine += jnp.where(hit, route_weights_ref[k : k + 1, :], 0.0)
    dispatch = dispatch.astype(jnp.bfloat16)
    coarse = combine.astype(jnp.bfloat16)
    fine = (combine - coarse.astype(jnp.float32)).astype(jnp.bfloat16)
    swap.wait()
    summed = mine[...].astype(jnp.float32) + theirs[...].astype(jnp.float32)
    resid[...] = (tokens_ref[...].astype(jnp.float32) + summed).astype(jnp.bfloat16)
    widened = resid[...].astype(jnp.float32)
    scale = lax.rsqrt(jnp.mean(widened * widened, axis=-1, keepdims=True) + 1e-06)
    my_half = pl.ds(pl.multiple_of(tp * half, half), half)
    other_half = pl.ds(pl.multiple_of((1 - tp) * half, half), half)
    normed = (resid[:, my_half].astype(jnp.float32) * scale * gain_ref[:, my_half]).astype(
        jnp.bfloat16
    )
    outgoing[...] = (
        jnp.dot(dispatch, normed, preferred_element_type=jnp.float32)
        .astype(jnp.bfloat16)
        .reshape(count, SLOT_TILE, half)
    )
    sends = []
    for step in range(1, count):
        other = lax.rem(ep + step, count)
        copy = remote(
            outgoing.at[other], near.at[ep], d_send.at[step], d_recv.at[step], (other, tp)
        )
        copy.start()
        sends.append(copy)
    near[ep] = outgoing[ep]
    forwards = []
    for step in range(count):
        source = lax.rem(ep + count - step, count)
        if step > 0:
            sends[step - 1].wait()
        copy = remote(
            near.at[source] if step > 0 else outgoing.at[ep],
            far.at[source],
            f_send.at[step],
            f_recv.at[step],
            partner,
        )
        copy.start()
        forwards.append(copy)
    for copy in loads:
        copy.wait()
    near_rows = near[...].reshape(slots, half)
    gate_pre = dot_t(near_rows, w_gate[:, my_half])
    up_pre = dot_t(near_rows, w_up[:, my_half])
    for copy in forwards:
        copy.wait()
    far_rows = far[...].reshape(slots, half)
    gate_pre += dot_t(far_rows, w_gate[:, other_half])
    up_pre += dot_t(far_rows, w_up[:, other_half])
    hidden = (gate_pre * jax.nn.sigmoid(gate_pre) * up_pre).astype(jnp.bfloat16)
    down_send[...] = jnp.dot(
        hidden, w_down[:, other_half], preferred_element_type=jnp.float32
    ).astype(jnp.bfloat16)
    swap = remote(down_send, down_recv, t_send.at[1], t_recv.at[1], partner)
    swap.start()
    kept = jnp.dot(hidden, w_down[:, my_half], preferred_element_type=jnp.float32).astype(
        jnp.bfloat16
    )
    swap.wait()
    finished[...] = (
        (kept.astype(jnp.float32) + down_recv[...].astype(jnp.float32))
        .astype(jnp.bfloat16)
        .reshape(count, SLOT_TILE, half)
    )
    sends = []
    for step in range(1, count):
        other = lax.rem(ep + step, count)
        copy = remote(
            finished.at[other], returned.at[ep], r_send.at[step], r_recv.at[step], (other, tp)
        )
        copy.start()
        sends.append(copy)
    returned[ep] = finished[ep]
    for copy in sends:
        copy.wait()
    back = returned[...].reshape(slots, half)
    turn = (((0,), (0,)), ((), ()))
    weighted = lax.dot_general(
        coarse, back, turn, preferred_element_type=jnp.float32
    ) + lax.dot_general(fine, back, turn, preferred_element_type=jnp.float32)
    last_send[...] = (resid[:, my_half].astype(jnp.float32) + weighted).astype(jnp.bfloat16)
    swap = remote(last_send, last_recv, t_send.at[2], t_recv.at[2], partner)
    swap.start()
    mixed_ref[:, my_half] = last_send[...]
    swap.wait()
    mixed_ref[:, other_half] = last_recv[...]


def mixer_call(tokens, mix_gain, weight_list, w_out):
    rows, width = tokens.shape
    w_query, w_key, w_value, w_outgate, w_igate, w_fgate = weight_list
    depth, columns = w_query.shape
    lines = lax.axis_size("ep") // PLANE
    heads = w_igate.shape[1]
    total = 4 * columns + LANES
    vmem = pl.BlockSpec(memory_space=pltpu.VMEM)
    anywhere = pl.BlockSpec(memory_space=pl.ANY)
    dma = pltpu.SemaphoreType.DMA
    bf = jnp.bfloat16
    planes = (PLANE, lines) + w_out.shape
    return pl.pallas_call(
        functools.partial(mixer_kernel, lines),
        out_shape=(
            jax.ShapeDtypeStruct((rows, total), jnp.float32),
            jax.ShapeDtypeStruct(planes, bf),
        ),
        in_specs=[anywhere] * 9,
        out_specs=(vmem, anywhere),
        scratch_shapes=[
            pltpu.VMEM((rows, width), bf),
            pltpu.VMEM((1, width), jnp.float32),
            pltpu.VMEM((heads, depth), bf),
            pltpu.VMEM((heads, depth), bf),
            pltpu.VMEM((LANES, depth), jnp.float32),
            pltpu.VMEM(planes, bf),
            pltpu.VMEM((rows, width), bf),
            pltpu.VMEM((lines, rows, depth * PLANE), bf),
            pltpu.VMEM((depth * PLANE, total), bf),
            pltpu.VMEM((lines, rows, total), jnp.float32),
            pltpu.VMEM((lines, rows, total), bf),
            pltpu.VMEM((lines, rows, total), bf),
            dma((9,)),
            dma((6,)),
            dma((6,)),
            dma((lines,)),
            dma((lines,)),
            dma((lines,)),
            dma((lines,)),
            dma((lines,)),
            dma((lines,)),
            dma((6,)),
            dma((6,)),
        ],
        compiler_params=pltpu.CompilerParams(
            collective_id=0, has_side_effects=True, vmem_limit_bytes=VMEM_BYTES
        ),
    )(
        tokens,
        mix_gain[None, :],
        w_query,
        w_key,
        w_value,
        w_outgate,
        jnp.swapaxes(w_igate, 0, 1),
        jnp.swapaxes(w_fgate, 0, 1),
        w_out,
    )


def cell_call(proj, igate_bias, fgate_bias, head_gain, state_matrix, state_norm, state_max):
    rows, heads, size, _ = state_matrix.shape
    wide = heads * size
    vmem = pl.BlockSpec(memory_space=pltpu.VMEM)
    anywhere = pl.BlockSpec(memory_space=pl.ANY)
    dma = pltpu.SemaphoreType.DMA
    f32 = jnp.float32
    cell_out, new_matrix, new_norm, new_max = pl.pallas_call(
        cell_kernel,
        out_shape=(
            jax.ShapeDtypeStruct((rows, wide), jnp.bfloat16),
            jax.ShapeDtypeStruct(state_matrix.shape, f32),
            jax.ShapeDtypeStruct(state_norm.shape, f32),
            jax.ShapeDtypeStruct((heads, rows), f32),
        ),
        in_specs=[vmem] + [anywhere] * 6,
        out_specs=(vmem, anywhere, vmem, vmem),
        scratch_shapes=[
            pltpu.VMEM((1, heads), f32),
            pltpu.VMEM((1, heads), f32),
            pltpu.VMEM((1, wide), f32),
            pltpu.VMEM(state_matrix.shape, f32),
            pltpu.VMEM(state_norm.shape, f32),
            pltpu.VMEM((heads, rows), f32),
            pltpu.VMEM((LANES, LANES), f32),
            pltpu.VMEM((rows, 2 * heads, size), f32),
            pltpu.VMEM((rows, 2 * heads, wide), f32),
            pltpu.VMEM((rows, 2 * heads, size), f32),
            pltpu.VMEM((rows, 2 * heads, size), f32),
            pltpu.VMEM((rows, 2 * heads, wide), f32),
            dma((5,)),
            dma((rows // 8,)),
            dma((rows // 8,)),
        ],
        compiler_params=pltpu.CompilerParams(vmem_limit_bytes=VMEM_BYTES),
    )(
        proj,
        igate_bias[None, :],
        fgate_bias[None, :],
        head_gain[None, :],
        state_matrix,
        state_norm,
        jnp.swapaxes(state_max, 0, 1),
    )
    return cell_out, new_matrix, new_norm, jnp.swapaxes(new_max, 0, 1)


def expert_call(
    cell_out, w_all, tokens, ffn_gain, routes, route_weights, w_gate, w_up, w_down
):
    rows, width = tokens.shape
    count = lax.axis_size("ep")
    gate_t = jnp.swapaxes(w_gate[0], 0, 1)
    up_t = jnp.swapaxes(w_up[0], 0, 1)
    down = w_down[0]
    half = width // 2
    area = count * SLOT_TILE
    vmem = pl.BlockSpec(memory_space=pltpu.VMEM)
    anywhere = pl.BlockSpec(memory_space=pl.ANY)
    dma = pltpu.SemaphoreType.DMA
    bf = jnp.bfloat16
    tile = (count, SLOT_TILE, half)
    return pl.pallas_call(
        functools.partial(expert_kernel, count),
        out_shape=jax.ShapeDtypeStruct((rows, width), bf),
        in_specs=[anywhere] * 9,
        out_specs=vmem,
        scratch_shapes=[
            pltpu.VMEM(cell_out.shape, bf),
            pltpu.VMEM(w_all.shape, bf),
            pltpu.VMEM((rows, width), bf),
            pltpu.VMEM((1, width), jnp.float32),
            pltpu.VMEM((routes.shape[1], rows), jnp.int32),
            pltpu.VMEM((routes.shape[1], rows), jnp.float32),
            pltpu.VMEM(gate_t.shape, bf),
            pltpu.VMEM(up_t.shape, bf),
            pltpu.VMEM(down.shape, bf),
            pltpu.VMEM((rows, width), bf),
            pltpu.VMEM((rows, width), bf),
            pltpu.VMEM((rows, width), bf),
            pltpu.VMEM(tile, bf),
            pltpu.VMEM(tile, bf),
            pltpu.VMEM(tile, bf),
            pltpu.VMEM((area, half), bf),
            pltpu.VMEM((area, half), bf),
            pltpu.VMEM(tile, bf),
            pltpu.VMEM(tile, bf),
            pltpu.VMEM((rows, half), bf),
            pltpu.VMEM((rows, half), bf),
            dma((9,)),
            dma((3,)),
            dma((3,)),
            dma((count,)),
            dma((count,)),
            dma((count,)),
            dma((count,)),
            dma((count,)),
            dma((count,)),
        ],
        compiler_params=pltpu.CompilerParams(
            collective_id=1, has_side_effects=True, vmem_limit_bytes=VMEM_BYTES
        ),
    )(
        cell_out,
        w_all,
        tokens,
        ffn_gain[None, :],
        jnp.swapaxes(routes, 0, 1),
        jnp.swapaxes(route_weights, 0, 1),
        gate_t,
        up_t,
        down,
    )


def rms_scale(values_in, gain_vec):
    widened = values_in.astype(jnp.float32)
    return (
        widened * lax.rsqrt(jnp.mean(widened * widened, axis=-1, keepdims=True) + 1e-06) * gain_vec
    )


def memory_cell(
    query,
    key_row,
    value_row,
    outgate,
    input_pre,
    forget_pre,
    head_gain,
    state_matrix,
    state_norm,
    state_max,
):
    seq_rows, head_count = input_pre.shape
    head_size = query.shape[1] // head_count
    query_heads = query.astype(jnp.float32).reshape(seq_rows, head_count, head_size)
    key_heads = key_row.astype(jnp.float32).reshape(
        seq_rows, head_count, head_size
    ) * head_size ** (-0.5)
    value_heads = value_row.astype(jnp.float32).reshape(seq_rows, head_count, head_size)
    log_forget = jax.nn.log_sigmoid(forget_pre)
    new_max = jnp.maximum(log_forget + state_max, input_pre)
    keep_old = jnp.exp(log_forget + state_max - new_max)
    keep_new = jnp.exp(input_pre - new_max)
    new_matrix = (
        keep_old[:, :, None, None] * state_matrix
        + keep_new[:, :, None, None] * value_heads[:, :, :, None] * key_heads[:, :, None, :]
    )
    new_norm = keep_old[:, :, None] * state_norm + keep_new[:, :, None] * key_heads
    numerator = jnp.einsum(
        "bhvd,bhd->bhv", new_matrix, query_heads, precision=lax.Precision.HIGHEST
    )
    denominator = jnp.sum(new_norm * query_heads, axis=-1)
    cell_read = numerator / jnp.maximum(jnp.abs(denominator), jnp.exp(-new_max))[:, :, None]
    centered = cell_read - jnp.mean(cell_read, axis=-1, keepdims=True)
    variance = jnp.mean(centered * centered, axis=-1, keepdims=True)
    scaled_cell = (centered * lax.rsqrt(variance + 1e-06)).reshape(seq_rows, head_count * head_size)
    cell_out = (scaled_cell * head_gain * jax.nn.sigmoid(outgate.astype(jnp.float32))).astype(
        jnp.bfloat16
    )
    return (cell_out, new_matrix, new_norm, new_max)


def kernels_fit(tokens, w_query, w_igate, w_out, w_expert_gate, routes):
    ep_count = lax.axis_size("ep")
    rows, width = tokens.shape
    capacity = max(2, 2 * rows * routes.shape[1] // (w_expert_gate.shape[0] * ep_count))
    return (
        lax.axis_size("tp") == 2
        and ep_count % (2 * PLANE) == 0
        and w_query.shape[0] == LANES
        and w_query.shape[1] % LANES == 0
        and w_out.shape[1] % LANES == 0
        and width % (2 * LANES) == 0
        and rows % SLOT_TILE == 0
        and w_igate.shape[1] == 4
        and rows <= LANES
        and w_expert_gate.shape[0] == 1
        and capacity <= SLOT_TILE
    )


def body(
    tokens,
    mix_gain,
    w_query,
    w_key,
    w_value,
    w_outgate,
    w_igate,
    w_fgate,
    igate_bias,
    fgate_bias,
    head_gain,
    w_out,
    state_matrix,
    state_norm,
    state_max,
    ffn_gain,
    w_expert_gate,
    w_expert_up,
    w_expert_down,
    routes,
    route_weights,
):
    seq_rows, width = tokens.shape
    weight_list = (w_query, w_key, w_value, w_outgate, w_igate, w_fgate)
    if kernels_fit(tokens, w_query, w_igate, w_out, w_expert_gate, routes):
        proj, w_all = mixer_call(tokens, mix_gain, weight_list, w_out)
        cell_out, new_matrix, new_norm, new_max = cell_call(
            proj, igate_bias, fgate_bias, head_gain, state_matrix, state_norm, state_max
        )
        mixed = expert_call(
            cell_out,
            w_all,
            tokens,
            ffn_gain,
            routes,
            route_weights,
            w_expert_gate,
            w_expert_up,
            w_expert_down,
        )
        return (mixed, new_matrix, new_norm, new_max)
    normed = rms_scale(tokens, mix_gain).astype(jnp.bfloat16)
    spread = lax.all_to_all(normed, "ep", split_axis=1, concat_axis=0, tiled=True)
    joined = jnp.concatenate(weight_list, axis=1)
    summed = lax.psum_scatter(
        jnp.dot(spread, joined, preferred_element_type=jnp.float32),
        "ep",
        scatter_dimension=0,
        tiled=True,
    )
    bounds = [0]
    for weight in weight_list:
        bounds.append(bounds[-1] + weight.shape[1])
    projected = tuple(
        (summed[:, bounds[index] : bounds[index + 1]] for index in range(len(weight_list)))
    )
    query = projected[0].astype(jnp.bfloat16)
    key_row = projected[1].astype(jnp.bfloat16)
    value_row = projected[2].astype(jnp.bfloat16)
    outgate = projected[3].astype(jnp.bfloat16)
    input_pre = projected[4] + igate_bias
    forget_pre = projected[5] + fgate_bias
    cell_out, new_matrix, new_norm, new_max = memory_cell(
        query,
        key_row,
        value_row,
        outgate,
        input_pre,
        forget_pre,
        head_gain,
        state_matrix,
        state_norm,
        state_max,
    )
    partial_out = jnp.dot(
        cell_out,
        lax.all_gather(w_out, "ep", axis=1, tiled=True),
        preferred_element_type=jnp.float32,
    )
    attended = lax.psum(partial_out.astype(jnp.bfloat16), "tp").astype(jnp.float32)
    resid = (tokens.astype(jnp.float32) + attended).astype(jnp.bfloat16)
    normed_two = rms_scale(resid, ffn_gain).astype(jnp.bfloat16)
    ep_count = lax.axis_size("ep")
    local_experts = w_expert_gate.shape[0]
    expert_total = local_experts * ep_count
    top_count = routes.shape[1]
    capacity = max(2, 2 * seq_rows * top_count // expert_total)
    flat_routes = routes.reshape(-1)
    onehot = (flat_routes[:, None] == jnp.arange(expert_total, dtype=jnp.int32)[None, :]).astype(
        jnp.int32
    )
    earlier = jnp.cumsum(onehot, axis=0, dtype=jnp.int32) - onehot
    slots = jnp.sum(onehot * earlier, axis=1, dtype=jnp.int32)
    targets = flat_routes * capacity + slots
    dispatch = (
        targets[:, None] == jnp.arange(expert_total * capacity, dtype=jnp.int32)[None, :]
    ).astype(jnp.bfloat16)
    route_rows = jnp.repeat(normed_two, top_count, axis=0)
    outgoing = jnp.einsum(
        "rs,rd->sd", dispatch, route_rows, preferred_element_type=jnp.float32
    ).astype(jnp.bfloat16)
    outgoing = outgoing.reshape(expert_total, capacity, width)
    received = lax.all_to_all(outgoing, "ep", split_axis=0, concat_axis=0, tiled=True)
    slot_count = received.shape[1]
    regrouped = received.reshape(ep_count, local_experts, slot_count, width)
    gate_pre = jnp.einsum(
        "nxcd,xdf->nxcf", regrouped, w_expert_gate, preferred_element_type=jnp.float32
    )
    up_pre = jnp.einsum(
        "nxcd,xdf->nxcf", regrouped, w_expert_up, preferred_element_type=jnp.float32
    )
    hidden = (jax.nn.silu(gate_pre) * up_pre).astype(jnp.bfloat16)
    partial_down = jnp.einsum(
        "nxcf,xfd->nxcd", hidden, w_expert_down, preferred_element_type=jnp.float32
    )
    expert_sum = lax.psum(partial_down.astype(jnp.bfloat16), "tp")
    finished = expert_sum.reshape(ep_count * local_experts, slot_count, width)
    returned = lax.all_to_all(finished, "ep", split_axis=0, concat_axis=0, tiled=True)
    picked = jnp.dot(
        dispatch,
        returned.reshape(expert_total * capacity, width),
        preferred_element_type=jnp.float32,
    )
    weighted = jnp.sum(
        picked.reshape(seq_rows, top_count, width) * route_weights[:, :, None], axis=1
    )
    mixed = (resid.astype(jnp.float32) + weighted).astype(jnp.bfloat16)
    return (mixed, new_matrix, new_norm, new_max)


def solution(mesh):
    placed = (
        P("ep", None),
        P(),
        P("ep", "tp"),
        P("ep", "tp"),
        P("ep", "tp"),
        P("ep", "tp"),
        P("ep", "tp"),
        P("ep", "tp"),
        P("tp"),
        P("tp"),
        P("tp"),
        P("tp", "ep"),
        P("ep", "tp", None, None),
        P("ep", "tp", None),
        P("ep", "tp"),
        P(),
        P("ep", None, "tp"),
        P("ep", None, "tp"),
        P("ep", "tp", None),
        P("ep", None),
        P("ep", None),
    )
    return jax.shard_map(
        body,
        mesh=mesh,
        in_specs=placed,
        out_specs=(P("ep", None), P("ep", "tp", None, None), P("ep", "tp", None), P("ep", "tp")),
        check_vma=False,
    )
```
